32 devices in a mesh: sp: 8 (over z, x), tp: 4 (over y, core).
Axes of the slice: x: 2, y: 2, z: 4, core: 2. Of those that a mesh axis runs over, the one named last changes fastest.
Arguments:
- queries: bfloat16 [6144, 2048], P('sp', 'tp'), may hold values from -110 to 110
- key_rows: bfloat16 [6144, 512], P('sp', 'tp'), may hold values from -4.5 to 4.5
- values: bfloat16 [6144, 512], P('sp', 'tp'), may hold values from -6 to 6
- sink_logits: float32 [32], P('tp'), may hold values from 2 to 7
- doc_ids: int32 [6144], P('sp'), may hold values from 0 to 3, as said below
- residual: bfloat16 [6144, 2048], P('sp'), may hold values from -20 to 20
- w_out: bfloat16 [2048, 2048], P('tp'), may hold values from -2.390625 to 2.390625
- norm_gain: float32 [2048], replicated, may hold values from 0.1 to 1.9
- w_value_up: bfloat16 [2048, 5632], P('sp', 'tp'), may hold values from -0.125 to 0.125
- w_gate_up: bfloat16 [2048, 5632], P('sp', 'tp'), may hold values from -0.125 to 0.125
- conv_taps: bfloat16 [3, 5632], P(None, 'tp'), may hold values from -3.5 to 3.5
- w_down_t: bfloat16 [2048, 5632], P('sp', 'tp'), may hold values from -0.078125 to 0.078125
Outputs:
- layer_out: bfloat16 [6144, 2048], P('sp', 'tp')
The draws below stay inside these ranges and needn't reach their ends.
Inputs may be any that keep to these rules, and one draw needn't show every extreme that they name: `doc_ids`: document numbers never fall along the sequence and every one of the 4 documents is present; each document has 2 or more positions.
All inputs are finite; a program needn't handle non-finite values.
Results may differ from the reference program's by a relative error of at most 0.017.
Values may be sent and summed in bfloat16 or wider, within the bound.
A program may use at most 64 MiB of HBM per device.

```python
import jax
import jax.numpy as jnp
from jax import lax

D = 2048
FF = 5632
HEADS = 32
KV_HEADS = 8
HEAD_DIM = 64
WINDOW = 128
TOK_DEV = 768
Q_W = 2048
SEQ = 6144
DOCS = 4
N_TP = 4


def paired_heads(key):
    key_part = jnp.clip(jax.random.normal(jax.random.fold_in(key, 11), (SEQ, KV_HEADS, HEAD_DIM), jnp.float32), -4.0, 4.0)
    query_part = jnp.clip(jax.random.normal(jax.random.fold_in(key, 12), (SEQ, HEADS, HEAD_DIM), jnp.float32), -5.0, 5.0)
    return (query_part.reshape(SEQ, HEADS * HEAD_DIM), key_part.reshape(SEQ, KV_HEADS * HEAD_DIM))


def draw_queries(key, part):
    return paired_heads(key)[0].astype(jnp.bfloat16)


def draw_key_rows(key, part):
    return paired_heads(key)[1].astype(jnp.bfloat16)


def draw_doc_ids(key, part):
    starts_count = DOCS - 1
    centre = 2 * TOK_DEV * (jnp.arange(starts_count, dtype=jnp.int32) + 1)
    offset = jax.random.randint(jax.random.fold_in(key, 31), (starts_count,), 1 - TOK_DEV, TOK_DEV, jnp.int32)
    starts = centre + offset
    position = jnp.arange(SEQ, dtype=jnp.int32)
    return jnp.sum((position[:, None] >= starts[None, :]).astype(jnp.int32), axis=1).astype(jnp.int32)


def draw_residual(key, part):
    column = jnp.arange(D).astype(jnp.float32)
    col_scale = 0.5 * jnp.exp(jnp.log(3.0) * column / (D - 1))
    draws_base = jnp.clip(jax.random.normal(jax.random.fold_in(key, 21), (SEQ, D), jnp.float32), -4.0, 4.0)
    return (draws_base * col_scale[None, :]).astype(jnp.bfloat16)


def level_of(rng, dims, shards, smallest, high):
    loudness, own = 1.0, jax.random.fold_in(rng, 6)
    for dim, blocks in shards:
        draws = jnp.exp(jax.random.uniform(jax.random.fold_in(own, dim), (blocks,), jnp.float32, smallest / len(shards), high / len(shards)))
        loudness = loudness * jnp.repeat(draws, dims[dim] // blocks).reshape([-1 if axis == dim else 1 for axis in range(len(dims))])
    return loudness


def scatter_about(stream_key, extent, deviation, most, split=(), held_as=jnp.bfloat16):
    values = jax.random.normal(stream_key, extent, jnp.float32) * deviation
    if len(split) > 0:
        values = level_of(stream_key, extent, split, -0.22, 0.18) * values
    return jnp.clip(values, min=-most, max=most).astype(held_as)


def setup_inputs(seed: int = 0) -> dict:
    key_of = jax.random.split(jax.random.key(seed), 13)
    return {
        "queries": draw_queries(jax.random.fold_in(key_of[12], 71), 0),
        "key_rows": draw_key_rows(jax.random.fold_in(key_of[12], 71), 0),
        "values": scatter_about(key_of[2], (SEQ, KV_HEADS * HEAD_DIM), 1.0, 6.0, ((0, 8), (1, 4))),
        "sink_logits": jnp.clip(2.0 + 5.0 * jax.random.uniform(key_of[3], (HEADS,), jnp.float32) ** level_of(key_of[3], (HEADS,), ((0, 4),), -0.2, 0.2), 2.0, 7.0),
        "doc_ids": draw_doc_ids(jax.random.fold_in(key_of[12], 71), 0),
        "residual": draw_residual(jax.random.fold_in(key_of[12], 71), 0),
        "w_out": scatter_about(key_of[6], (Q_W, D), 0.4, 2.390625, ((0, 4),)),
        "norm_gain": jnp.clip(1.0 + 0.18 * jax.random.normal(key_of[7], (D,), jnp.float32), 0.1, 1.9),
        "w_value_up": scatter_about(key_of[8], (D, FF), D ** -0.5, 0.125, ((0, 8), (1, 4))),
        "w_gate_up": scatter_about(key_of[9], (D, FF), D ** -0.5, 0.125, ((0, 8), (1, 4))),
        "conv_taps": scatter_about(key_of[10], (3, FF), 3 ** -0.5, 3.5, ((1, 4),)),
        "w_down_t": scatter_about(key_of[11], (D, FF), FF ** -0.5, 0.078125, ((0, 8), (1, 4))),
    }


EPS = 1e-06
NEG = -1e+30

def attend_block(q_block, kv_window, doc_window, doc_query, sink_logits):
    per_kv = HEADS // KV_HEADS
    kv_cols = KV_HEADS * HEAD_DIM
    q_heads = q_block.astype(jnp.float32).reshape(WINDOW, KV_HEADS, per_kv, HEAD_DIM)
    k_heads = kv_window[:, :kv_cols].astype(jnp.float32).reshape(3 * WINDOW, KV_HEADS, HEAD_DIM)
    v_heads = kv_window[:, kv_cols:].astype(jnp.float32).reshape(3 * WINDOW, KV_HEADS, HEAD_DIM)
    score = jnp.einsum('qkgd,jkd->kgqj', q_heads, k_heads) * HEAD_DIM ** (-0.5)
    offsets = jnp.arange(3 * WINDOW)[None, :] - WINDOW - jnp.arange(WINDOW)[:, None]
    allowed = (jnp.abs(offsets) <= WINDOW) & (doc_query[:, None] == doc_window[None, :])
    sink_grid = sink_logits.reshape(KV_HEADS, per_kv)[:, :, None]
    highest = jnp.maximum(lax.optimization_barrier(jnp.max(jnp.where(allowed, score, NEG), axis=-1)), sink_grid)
    raw = jnp.where(allowed, jnp.exp(score - highest[..., None]), 0.0)
    total = lax.optimization_barrier(jnp.sum(raw, axis=-1)) + jnp.exp(sink_grid - highest)
    probs = (raw / total[..., None]).astype(jnp.bfloat16)
    attended = jnp.einsum('kgqj,jkd->qkgd', probs.astype(jnp.float32), v_heads)
    return attended.reshape(WINDOW, HEADS * HEAD_DIM).astype(jnp.bfloat16)

def rounded(term):
    return lax.optimization_barrier(term.astype(jnp.bfloat16)).astype(jnp.float32)

def reference(queries, key_rows, values, sink_logits, doc_ids, residual, w_out, norm_gain, w_value_up, w_gate_up, conv_taps, w_down_t):
    seq_len = queries.shape[0]
    blocks = seq_len // WINDOW
    stacked = jnp.concatenate([key_rows, values], axis=1)
    padded = jnp.pad(stacked, ((WINDOW, WINDOW), (0, 0)))
    labels = doc_ids + 1
    label_pad = jnp.pad(labels, (WINDOW, WINDOW))
    kv_blocks = padded.reshape(blocks + 2, WINDOW, stacked.shape[1])
    kv_window = jnp.concatenate([kv_blocks[:-2], kv_blocks[1:-1], kv_blocks[2:]], axis=1)
    lab_blocks = label_pad.reshape(blocks + 2, WINDOW)
    doc_window = jnp.concatenate([lab_blocks[:-2], lab_blocks[1:-1], lab_blocks[2:]], axis=1)
    q_blocks = queries.reshape(blocks, WINDOW, queries.shape[1])
    doc_query = labels.reshape(blocks, WINDOW)
    attended = lax.map(lambda items: attend_block(items[0], items[1], items[2], items[3], sink_logits), (q_blocks, kv_window, doc_window, doc_query))
    attended = attended.reshape(seq_len, queries.shape[1])
    head_cols = queries.shape[1] // N_TP
    attn_total = jnp.zeros((seq_len, D), jnp.float32)
    for member in range(N_TP):
        cols = attended[:, member * head_cols:(member + 1) * head_cols]
        rows_w = w_out[member * head_cols:(member + 1) * head_cols]
        attn_total = attn_total + rounded(jnp.dot(cols, rows_w, preferred_element_type=jnp.float32))
    mixed = (residual.astype(jnp.float32) + attn_total).astype(jnp.bfloat16)
    mixed_f = mixed.astype(jnp.float32)
    mean_sq = lax.optimization_barrier(jnp.mean(mixed_f * mixed_f, axis=1, keepdims=True))
    normed = (mixed_f * lax.rsqrt(mean_sq + EPS) * norm_gain).astype(jnp.bfloat16)
    up_value = jnp.dot(normed, w_value_up, preferred_element_type=jnp.float32).astype(jnp.bfloat16)
    up_gate = jnp.dot(normed, w_gate_up, preferred_element_type=jnp.float32).astype(jnp.bfloat16)
    value_f = up_value.astype(jnp.float32)
    value_pad = jnp.pad(value_f, ((1, 1), (0, 0)))
    lab_one = jnp.pad(labels, (1, 1))
    prev_same = (lab_one[:-2] == labels)[:, None]
    next_same = (lab_one[2:] == labels)[:, None]
    tap_f = conv_taps.astype(jnp.float32)
    conv = tap_f[0] * jnp.where(prev_same, value_pad[:-2], 0.0) + tap_f[1] * value_f + tap_f[2] * jnp.where(next_same, value_pad[2:], 0.0)
    hidden = (jax.nn.silu(conv) * up_gate.astype(jnp.float32)).astype(jnp.bfloat16)
    ff_cols = FF // N_TP
    ffn_total = jnp.zeros((seq_len, D), jnp.float32)
    for member in range(N_TP):
        cols = hidden[:, member * ff_cols:(member + 1) * ff_cols]
        down_cols = w_down_t[:, member * ff_cols:(member + 1) * ff_cols]
        term = lax.dot_general(cols, down_cols, (((1,), (1,)), ((), ())), preferred_element_type=jnp.float32)
        ffn_total = ffn_total + rounded(term)
    return (mixed.astype(jnp.float32) + ffn_total).astype(jnp.bfloat16)
```

```python
import functools

import jax
import jax.numpy as jnp
from jax import lax
from jax.experimental import pallas as pl
from jax.experimental.pallas import tpu as pltpu
from jax.sharding import PartitionSpec as P

HEAD_DIM = 64
WINDOW = 128
EPS = 1e-06
NEG = -1e30
RIM = 16
MESH = pl.DeviceIdType.MESH
F32 = jnp.float32
BF16 = jnp.bfloat16


def kernel(
    n, ntp,
    q_ref, k_ref, v_ref, sink_ref, lab_row_ref, lab_col_ref, prev_ok_ref, next_ok_ref,
    res_hbm, wout_ref, gain_ref, wv_hbm, wg_hbm, taps_ref, wd_hbm,
    out_ref,
    up, down, kx, vx, lx, part, first, second, mixed, normed, value, gate, rim, pd, res,
    loc_sem, ring_send, ring_recv, halo_send, halo_recv, rim_send, rim_recv,
    core_send, core_recv, y_send, y_recv, back_send, back_recv, pair_send, pair_recv,
    dcore_send, dcore_recv, dy_send, dy_recv,
):
    me = lax.axis_index("sp")
    tp = lax.axis_index("tp")
    core = lax.rem(tp, 2)
    y = tp // 2
    ny = ntp // 2
    partner = y * 2 + 1 - core
    rows = q_ref.shape[0]
    half = rows // 2
    piece = half // ny
    block = wv_hbm.shape[0]
    depth = block // 2
    quarter = block // 4

    def place(p):
        h = p // (n // 2)
        return (1 - h) * (2 * p) + h * (2 * n - 1 - 2 * p)

    odd = lax.rem(me, 2)
    pos = (1 - odd) * (me // 2) + odd * ((2 * n - 1 - me) // 2)
    ahead = place(lax.rem(pos + 1, n))
    behind = place(lax.rem(pos + n - 1, n))
    right = lax.rem(me + 1, n)
    left = lax.rem(me + n - 1, n)

    loads = []
    for i, (src, dst) in enumerate((
        (wv_hbm, up.at[0, pl.ds(me * block, block)]),
        (wg_hbm, up.at[1, pl.ds(me * block, block)]),
        (wd_hbm, down.at[pl.ds(me * block, block)]),
        (res_hbm.at[pl.ds(core * half + y * piece, piece)], res),
    )):
        c = pltpu.make_async_copy(src, dst, loc_sem.at[i])
        c.start()
        loads.append(c)

    barrier = pltpu.get_barrier_semaphore()
    peers = [(ahead, tp), (behind, tp), (right, tp), (left, tp), (me, partner)]
    for j in range(1, ny):
        peers.append((me, lax.rem(y + j, ny) * 2 + core))
    for peer in peers:
        pl.semaphore_signal(barrier, inc=1, device_id=peer, device_id_type=MESH)
    for c in loads:
        c.wait()
    pl.semaphore_wait(barrier, len(peers))

    def spot(stream, way, owner):
        if stream < 2:
            return up.at[stream, pl.ds(owner * block + way * depth, depth)]
        return down.at[pl.ds(owner * block + way * depth + (stream - 2) * quarter, quarter)]

    def ring(stream, way, s, arriving):
        shift = s + 1 if arriving else s
        owner = place(lax.rem(pos + n - shift, n)) if way == 0 else place(lax.rem(pos + shift, n))
        ref = spot(stream, way, owner)
        return pltpu.make_async_remote_copy(
            src_ref=ref, dst_ref=ref,
            send_sem=ring_send.at[stream, way, s], recv_sem=ring_recv.at[stream, way, s],
            device_id=(ahead if way == 0 else behind, tp), device_id_type=MESH,
        )

    def begin(stream):
        for way in range(2):
            ring(stream, way, 0, False).start()

    def forward(stream, s, last=False):
        for way in range(2):
            ring(stream, way, s, True).wait_recv()
            if not last:
                ring(stream, way, s + 1, False).start()

    queue = []
    for s in range(n - 1):
        for stream in (0, 1):
            queue.append((stream, s))
    for s in range(n - 1):
        for stream in (2, 3):
            queue.append((stream, s))
    done = [0]

    def serve(count):
        for _ in range(count):
            if done[0] == len(queue):
                return
            stream, s = queue[done[0]]
            done[0] += 1
            forward(stream, s, last=s == n - 2)
            if stream < 2 and s == n - 2:
                begin(stream + 2)

    halo = []

    def remote(src, dst, send, recv, where):
        c = pltpu.make_async_remote_copy(
            src_ref=src, dst_ref=dst, send_sem=send, recv_sem=recv, device_id=where, device_id_type=MESH
        )
        c.start()
        return c

    ends = pl.ds(rows - WINDOW, WINDOW)
    starts = pl.ds(0, WINDOW)
    low, high = pl.ds(0, WINDOW), pl.ds(rows + WINDOW, WINDOW)
    for i, (src, dst) in enumerate(((k_ref, kx), (v_ref, vx))):
        halo.append(remote(src.at[ends], dst.at[low], halo_send.at[i, 0], halo_recv.at[i, 0], (right, tp)))
        halo.append(remote(src.at[starts], dst.at[high], halo_send.at[i, 1], halo_recv.at[i, 1], (left, tp)))
    halo.append(remote(lab_row_ref.at[:, ends], lx.at[:, low], halo_send.at[2, 0], halo_recv.at[2, 0], (right, tp)))
    halo.append(remote(lab_row_ref.at[:, starts], lx.at[:, high], halo_send.at[2, 1], halo_recv.at[2, 1], (left, tp)))
    begin(0)
    begin(1)
    inner = pl.ds(WINDOW, rows)
    kx[inner, :] = k_ref[...]
    vx[inner, :] = v_ref[...]
    lx[:, inner] = lab_row_ref[...]
    for c in halo:
        c.wait()

    kv_local = k_ref.shape[1] // HEAD_DIM
    per_kv = q_ref.shape[1] // k_ref.shape[1]
    blocks = rows // WINDOW
    model = wout_ref.shape[1]

    def attend(b, carry):
        here = pl.ds(pl.multiple_of(b * WINDOW, WINDOW), WINDOW)
        wide = pl.ds(pl.multiple_of(b * WINDOW, WINDOW), 3 * WINDOW)
        q = q_ref[here, :]
        kw = kx[wide, :]
        vw = vx[wide, :]
        lab_k = lx[0:1, wide]
        lab_q = lab_col_ref[here, :]
        key = lax.broadcasted_iota(jnp.int32, (WINDOW, 3 * WINDOW), 1) - WINDOW
        query = lax.broadcasted_iota(jnp.int32, (WINDOW, 3 * WINDOW), 0)
        at = key + me * rows + b * WINDOW
        allowed = (jnp.abs(key - query) <= WINDOW) & (lab_q == lab_k) & (at >= 0) & (at < n * rows)
        results = []
        for g in range(kv_local):
            k = kw[:, g * HEAD_DIM:(g + 1) * HEAD_DIM]
            v = vw[:, g * HEAD_DIM:(g + 1) * HEAD_DIM]
            for j in range(per_kv):
                h = g * per_kv + j
                qh = q[:, h * HEAD_DIM:(h + 1) * HEAD_DIM]
                score = lax.dot_general(
                    qh, k, (((1,), (1,)), ((), ())), preferred_element_type=F32
                ) * HEAD_DIM ** (-0.5)
                score = jnp.where(allowed, score, NEG)
                sink = sink_ref[h]
                highest = jnp.maximum(jnp.max(score, axis=1, keepdims=True), sink)
                raw = jnp.where(allowed, jnp.exp(score - highest), 0.0)
                total = jnp.sum(raw, axis=1, keepdims=True) + jnp.exp(sink - highest)
                probs = (raw / total).astype(BF16)
                results.append(jnp.dot(probs, v, preferred_element_type=F32).astype(BF16))
        attended = jnp.concatenate(results, axis=1)
        part[here, :] = jnp.dot(attended, wout_ref[...], preferred_element_type=F32).astype(BF16)
        return carry

    split = blocks // 3
    for t in range(3):
        lax.fori_loop(t * split, (t + 1) * split if t < 2 else blocks, attend, 0)
        serve(1)

    tile = 32
    other_half = pl.ds((1 - core) * half, half)
    swap = remote(part.at[other_half], first, core_send, core_recv, (me, partner))
    swap.wait()

    def add_first(i, carry):
        r = pl.ds(pl.multiple_of(i * tile, tile), tile)
        o = pl.ds(pl.multiple_of(core * half + i * tile, tile), tile)
        first[r, :] = (part[o, :].astype(F32) + first[r, :].astype(F32)).astype(BF16)
        return carry

    lax.fori_loop(0, half // tile, add_first, 0)
    copies = []
    for j in range(1, ny):
        to = lax.rem(y + j, ny)
        copies.append(remote(
            first.at[pl.ds(to * piece, piece)], second.at[j - 1], y_send.at[j - 1], y_recv.at[j - 1], (me, to * 2 + core)
        ))
    serve(2)
    for c in copies:
        c.wait()

    def add_second(i, carry):
        r = pl.ds(pl.multiple_of(i * tile, tile), tile)
        s = first[pl.ds(pl.multiple_of(y * piece + i * tile, tile), tile), :].astype(F32)
        for j in range(ny - 1):
            s = s + second[j, r, :].astype(F32)
        o = pl.ds(pl.multiple_of(core * half + y * piece + i * tile, tile), tile)
        mixed[o, :] = (res[r, :].astype(F32) + s).astype(BF16)
        return carry

    lax.fori_loop(0, piece // tile, add_second, 0)
    mine = mixed.at[pl.ds(core * half + y * piece, piece)]
    copies = []
    for j in range(1, ny):
        to = lax.rem(y + j, ny)
        copies.append(remote(mine, mine, back_send.at[j - 1], back_recv.at[j - 1], (me, to * 2 + core)))
    serve(2)
    for j, c in enumerate(copies):
        c.wait_send()
        frm = lax.rem(y + ny - (j + 1), ny)
        theirs = mixed.at[pl.ds(core * half + frm * piece, piece)]
        pltpu.make_async_remote_copy(
            src_ref=theirs, dst_ref=theirs, send_sem=back_send.at[j], recv_sem=back_recv.at[j],
            device_id=(me, partner), device_id_type=MESH,
        ).wait_recv()
    own_half = mixed.at[pl.ds(core * half, half)]
    swap = remote(own_half, own_half, pair_send, pair_recv, (me, partner))
    swap.wait_send()
    their_half = mixed.at[other_half]
    pltpu.make_async_remote_copy(
        src_ref=their_half, dst_ref=their_half, send_sem=pair_send, recv_sem=pair_recv,
        device_id=(me, partner), device_id_type=MESH,
    ).wait_recv()

    def normalise(i, carry):
        r = pl.ds(pl.multiple_of(i * tile, tile), tile)
        m = mixed[r, :].astype(F32)
        mean_sq = jnp.mean(m * m, axis=1, keepdims=True)
        normed[r, :] = (m * lax.rsqrt(mean_sq + EPS) * gain_ref[...]).astype(BF16)
        return carry

    lax.fori_loop(0, rows // tile, normalise, 0)

    serve(2 * (n - 1) - done[0])
    big = rows // 3

    def project(i, carry):
        r = pl.ds(pl.multiple_of(i * big, big), big)
        value[r, :] = jnp.dot(normed[r, :], up[0], preferred_element_type=F32).astype(BF16)
        gate[r, :] = jnp.dot(normed[r, :], up[1], preferred_element_type=F32).astype(BF16)
        return carry

    for t in range(3):
        lax.fori_loop(t, t + 1, project, 0)
        serve(2)

    tail = remote(value.at[pl.ds(rows - RIM, RIM)], rim.at[0], rim_send.at[0], rim_recv.at[0], (right, tp))
    head = remote(value.at[pl.ds(0, RIM)], rim.at[1], rim_send.at[1], rim_recv.at[1], (left, tp))
    tail.wait()
    head.wait()
    serve(1)

    taps = taps_ref[...].astype(F32)
    step = 64
    before = rim[0, RIM - 1:RIM, :].astype(F32)
    for i in range(rows // step):
        r = slice(i * step, (i + 1) * step)
        x = value[r, :].astype(F32)
        after = (value[(i + 1) * step:(i + 1) * step + RIM, :] if (i + 1) * step < rows else rim[1, :, :])[0:1].astype(F32)
        prev = jnp.concatenate([before, x[:-1]], axis=0)
        nxt = jnp.concatenate([x[1:], after], axis=0)
        conv = (
            taps[0:1] * jnp.where(prev_ok_ref[r, :] > 0, prev, 0.0)
            + taps[1:2] * x
            + taps[2:3] * jnp.where(next_ok_ref[r, :] > 0, nxt, 0.0)
        )
        gate[r, :] = (conv * jax.nn.sigmoid(conv) * gate[r, :].astype(F32)).astype(BF16)
        before = x[step - 1:step]
        if i % 4 == 3:
            serve(1)
    serve(len(queue))

    span = model // ntp

    def lower(t):
        def body(i, carry):
            r = pl.ds(pl.multiple_of(i * big, big), big)
            w = down[pl.ds(pl.multiple_of(t * span, span), span), :]
            pd[t, r, :] = lax.dot_general(
                gate[r, :], w, (((1,), (1,)), ((), ())), preferred_element_type=F32
            ).astype(BF16)
            return carry

        lax.fori_loop(0, 3, body, 0)

    inbox = part
    across = []
    for j in range(1, ny + 1):
        yy = lax.rem(y + j, ny)
        t = yy * 2 + 1 - core
        lower(t)
        across.append(remote(pd.at[t], second_in(inbox, yy, span), dcore_send.at[j - 1], dcore_recv.at[j - 1], (me, partner)))
    copies = []
    for j in range(1, ny + 1):
        yy = lax.rem(y + j, ny)
        t = yy * 2 + core
        lower(t)
        across[j - 1].wait()
        box = second_in(inbox, yy, span)

        def merge(i, carry):
            r = pl.ds(pl.multiple_of(i * 64, 64), 64)
            pd[t, r, :] = (pd[t, r, :].astype(F32) + box[r, :].astype(F32)).astype(BF16)
            return carry

        lax.fori_loop(0, rows // 64, merge, 0)
        if j < ny:
            to = yy * 2 + core
            copies.append(remote(
                pd.at[t], part.at[:, pl.ds((ny + j - 1) * span, span)], dy_send.at[j - 1], dy_recv.at[j - 1], (me, to)
            ))
    for c in copies:
        c.wait()

    def finish(i, carry):
        r = pl.ds(pl.multiple_of(i * 64, 64), 64)
        s = pd[tp, r, :].astype(F32)
        for j in range(ny - 1):
            s = s + part[r, (ny + j) * span:(ny + j + 1) * span].astype(F32)
        out_ref[r, :] = (mixed[r, pl.ds(pl.multiple_of(tp * span, span), span)].astype(F32) + s).astype(BF16)
        return carry

    lax.fori_loop(0, rows // 64, finish, 0)
    for stream in range(4):
        for way in range(2):
            for s in range(n - 1):
                ring(stream, way, s, False).wait_send()


def second_in(ref, slot, span):
    return ref.at[:, pl.ds(pl.multiple_of(slot * span, span), span)]


def solution(mesh):
    n, ntp = mesh.shape["sp"], mesh.shape["tp"]

    def per_device(q, k, v, sink, doc, res, wout, gain, wv, wg, taps, wd):
        rows, model = res.shape
        hidden = wv.shape[1]
        block = wv.shape[0]
        ny = ntp // 2
        edge_fwd = [(i, i + 1) for i in range(n - 1)]
        edge_bwd = [(b, a) for a, b in edge_fwd]
        labels = doc + 1
        before = lax.ppermute(labels[-1:], "sp", edge_fwd)
        after = lax.ppermute(labels[:1], "sp", edge_bwd)
        padded = jnp.concatenate([before, labels, after])
        prev_ok = (padded[:-2] == labels).astype(F32)[:, None]
        next_ok = (padded[2:] == labels).astype(F32)[:, None]
        lab_row = jnp.broadcast_to(labels[None, :], (8, rows))
        vm = pl.BlockSpec(memory_space=pltpu.VMEM)
        hbm = pl.BlockSpec(memory_space=pl.ANY)
        smem = pl.BlockSpec(memory_space=pltpu.SMEM)
        dma = pltpu.SemaphoreType.DMA
        kvc = k.shape[1]
        span = model // ntp
        scratch = [
            pltpu.VMEM((2, n * block, hidden), BF16),
            pltpu.VMEM((n * block, hidden), BF16),
            pltpu.VMEM((rows + 2 * WINDOW, kvc), BF16),
            pltpu.VMEM((rows + 2 * WINDOW, kvc), BF16),
            pltpu.VMEM((8, rows + 2 * WINDOW), jnp.int32),
            pltpu.VMEM((rows, model), BF16),
            pltpu.VMEM((rows // 2, model), BF16),
            pltpu.VMEM((max(ny - 1, 1), rows // 2 // ny, model), BF16),
            pltpu.VMEM((rows, model), BF16),
            pltpu.VMEM((rows, model), BF16),
            pltpu.VMEM((rows, hidden), BF16),
            pltpu.VMEM((rows, hidden), BF16),
            pltpu.VMEM((2, RIM, hidden), BF16),
            pltpu.VMEM((ntp, rows, span), BF16),
            pltpu.VMEM((rows // 2 // ny, model), BF16),
            dma((4,)),
            dma((4, 2, n - 1)), dma((4, 2, n - 1)),
            dma((3, 2)), dma((3, 2)),
            dma((2,)), dma((2,)),
            dma, dma,
            dma((ny,)), dma((ny,)),
            dma((ny,)), dma((ny,)),
            dma, dma,
            dma((ny,)), dma((ny,)),
            dma((ny,)), dma((ny,)),
        ]
        return pl.pallas_call(
            functools.partial(kernel, n, ntp),
            out_shape=jax.ShapeDtypeStruct((rows, span), BF16),
            in_specs=[vm, vm, vm, smem, vm, vm, vm, vm, hbm, vm, vm, hbm, hbm, vm, hbm],
            out_specs=vm,
            scratch_shapes=scratch,
            compiler_params=pltpu.CompilerParams(
                collective_id=0, has_side_effects=True, vmem_limit_bytes=67043328
            ),
            name="layer",
        )(q, k, v, sink, lab_row, labels[:, None], prev_ok, next_ok, res, wout, gain[None, :], wv, wg, taps, wd)

    placed = (
        P("sp", "tp"), P("sp", "tp"), P("sp", "tp"), P("tp"), P("sp"), P("sp", None),
        P("tp", None), P(), P("sp", "tp"), P("sp", "tp"), P(None, "tp"), P("sp", "tp"),
    )
    return jax.shard_map(
        per_device, mesh=mesh, in_specs=placed, out_specs=P("sp", "tp"), check_vma=False
    )
```

```python
import functools

import jax
import jax.numpy as jnp
from jax import lax
from jax.experimental import pallas as pl
from jax.experimental.pallas import tpu as pltpu
from jax.sharding import PartitionSpec as P

HEAD_DIM = 64
WINDOW = 128
EPS = 1e-06
NEG = -1e30
RIM = 16
MESH = pl.DeviceIdType.MESH
F32 = jnp.float32
BF16 = jnp.bfloat16


def kernel(
    n, ntp,
    q_ref, k_ref, v_ref, sink_ref, lab_row_ref,
    res_hbm, wout_ref, gain_ref, wv_hbm, wg_hbm, taps_ref, wd_hbm,
    out_ref,
    up, down, kx, vx, lx, lc, part, first, second, mixed, normed, value, gate, rim, pd, box, inbox, res,
    loc_sem, ring_send, ring_recv, halo_send, halo_recv, rim_send, rim_recv,
    core_send, core_recv, y_send, y_recv, back_send, back_recv, pair_send, pair_recv,
    down_send, down_recv, out_send, out_recv,
):
    me = lax.axis_index("sp")
    tp = lax.axis_index("tp")
    core = lax.rem(tp, 2)
    y = tp // 2
    ny = ntp // 2
    partner = y * 2 + 1 - core
    rows = q_ref.shape[0]
    half = rows // 2
    piece = half // ny
    block = wv_hbm.shape[0]
    depth = block // 2
    quarter = block // 4

    def place(p):
        h = p // (n // 2)
        return (1 - h) * (2 * p) + h * (2 * n - 1 - 2 * p)

    odd = lax.rem(me, 2)
    pos = (1 - odd) * (me // 2) + odd * ((2 * n - 1 - me) // 2)
    ahead = place(lax.rem(pos + 1, n))
    behind = place(lax.rem(pos + n - 1, n))
    right = lax.rem(me + 1, n)
    left = lax.rem(me + n - 1, n)

    loads = []
    for i, (src, dst) in enumerate((
        (wv_hbm, up.at[0, pl.ds(me * block, block)]),
        (wg_hbm, up.at[1, pl.ds(me * block, block)]),
        (wd_hbm, down.at[pl.ds(me * block, block)]),
        (res_hbm.at[pl.ds(core * half + y * piece, piece)], res),
    )):
        c = pltpu.make_async_copy(src, dst, loc_sem.at[i])
        c.start()
        loads.append(c)

    barrier = pltpu.get_barrier_semaphore()
    peers = [(ahead, tp), (behind, tp), (right, tp), (left, tp)]
    for j in range(1, ntp):
        peers.append((me, lax.rem(tp + j, ntp)))
    for peer in peers:
        pl.semaphore_signal(barrier, inc=1, device_id=peer, device_id_type=MESH)
    for c in loads:
        c.wait()
    pl.semaphore_wait(barrier, len(peers))

    def spot(stream, way, owner):
        if stream < 2:
            return up.at[stream, pl.ds(owner * block + way * depth, depth)]
        return down.at[pl.ds(owner * block + way * depth + (stream - 2) * quarter, quarter)]

    def ring(stream, way, s, arriving):
        shift = s + 1 if arriving else s
        owner = place(lax.rem(pos + n - shift, n)) if way == 0 else place(lax.rem(pos + shift, n))
        ref = spot(stream, way, owner)
        return pltpu.make_async_remote_copy(
            src_ref=ref, dst_ref=ref,
            send_sem=ring_send.at[stream, way, s], recv_sem=ring_recv.at[stream, way, s],
            device_id=(ahead if way == 0 else behind, tp), device_id_type=MESH,
        )

    def begin(stream):
        for way in range(2):
            ring(stream, way, 0, False).start()

    def forward(stream, s, last=False):
        for way in range(2):
            ring(stream, way, s, True).wait_recv()
            if not last:
                ring(stream, way, s + 1, False).start()

    queue = []
    for s in range(n - 1):
        for stream in (0, 1):
            queue.append((stream, s))
    for s in range(n - 1):
        for stream in (2, 3):
            queue.append((stream, s))
    done = [0]

    def serve(count):
        for _ in range(count):
            if done[0] == len(queue):
                return
            stream, s = queue[done[0]]
            done[0] += 1
            forward(stream, s, last=s == n - 2)
            if stream < 2 and s == n - 2:
                begin(stream + 2)

    halo = []

    def remote(src, dst, send, recv, where):
        c = pltpu.make_async_remote_copy(
            src_ref=src, dst_ref=dst, send_sem=send, recv_sem=recv, device_id=where, device_id_type=MESH
        )
        c.start()
        return c

    ends = pl.ds(rows - WINDOW, WINDOW)
    starts = pl.ds(0, WINDOW)
    low, high = pl.ds(0, WINDOW), pl.ds(rows + WINDOW, WINDOW)
    for i, (src, dst) in enumerate(((k_ref, kx), (v_ref, vx))):
        halo.append(remote(src.at[ends], dst.at[low], halo_send.at[i, 0], halo_recv.at[i, 0], (right, tp)))
        halo.append(remote(src.at[starts], dst.at[high], halo_send.at[i, 1], halo_recv.at[i, 1], (left, tp)))
    halo.append(remote(lab_row_ref.at[:, ends], lx.at[:, low], halo_send.at[2, 0], halo_recv.at[2, 0], (right, tp)))
    halo.append(remote(lab_row_ref.at[:, starts], lx.at[:, high], halo_send.at[2, 1], halo_recv.at[2, 1], (left, tp)))
    begin(0)
    begin(1)
    inner = pl.ds(WINDOW, rows)
    kx[inner, :] = k_ref[...]
    vx[inner, :] = v_ref[...]
    lx[:, inner] = lab_row_ref[...]
    for c in halo:
        c.wait()
    lx[:, low] = jnp.where(me == 0, -1, lx[:, low])
    lx[:, high] = jnp.where(me == n - 1, -1, lx[:, high])
    for i in range(rows // WINDOW + 2):
        chunk = slice(i * WINDOW, (i + 1) * WINDOW)
        square = jnp.broadcast_to(lx[0:1, chunk].astype(F32), (WINDOW, WINDOW))
        lc[chunk, :] = jnp.transpose(square)

    kv_local = k_ref.shape[1] // HEAD_DIM
    per_kv = q_ref.shape[1] // k_ref.shape[1]
    blocks = rows // WINDOW
    model = wout_ref.shape[1]

    def attend(b, carry):
        here = pl.ds(pl.multiple_of(b * WINDOW, WINDOW), WINDOW)
        wide = pl.ds(pl.multiple_of(b * WINDOW, WINDOW), 3 * WINDOW)
        q = q_ref[here, :]
        kw = kx[wide, :]
        vw = vx[wide, :]
        lab_k = lx[0:1, wide].astype(F32)
        lab_q = lc[pl.ds(pl.multiple_of(b * WINDOW + WINDOW, WINDOW), WINDOW), 0:1]
        key = lax.broadcasted_iota(jnp.int32, (WINDOW, 3 * WINDOW), 1) - WINDOW
        query = lax.broadcasted_iota(jnp.int32, (WINDOW, 3 * WINDOW), 0)
        allowed = (jnp.abs(key - query) <= WINDOW) & (lab_q == lab_k)
        results = []
        for g in range(kv_local):
            k = kw[:, g * HEAD_DIM:(g + 1) * HEAD_DIM]
            v = vw[:, g * HEAD_DIM:(g + 1) * HEAD_DIM]
            for j in range(per_kv):
                h = g * per_kv + j
                qh = q[:, h * HEAD_DIM:(h + 1) * HEAD_DIM]
                score = lax.dot_general(
                    qh, k, (((1,), (1,)), ((), ())), preferred_element_type=F32
                ) * HEAD_DIM ** (-0.5)
                score = jnp.where(allowed, score, NEG)
                sink = sink_ref[h]
                highest = jnp.maximum(jnp.max(score, axis=1, keepdims=True), sink)
                raw = jnp.where(allowed, jnp.exp(score - highest), 0.0)
                total = jnp.sum(raw, axis=1, keepdims=True) + jnp.exp(sink - highest)
                probs = (raw / total).astype(BF16)
                results.append(jnp.dot(probs, v, preferred_element_type=F32).astype(BF16))
        attended = jnp.concatenate(results, axis=1)
        part[here, :] = jnp.dot(attended, wout_ref[...], preferred_element_type=F32).astype(BF16)
        return carry

    split = blocks // 3
    for t in range(3):
        lax.fori_loop(t * split, (t + 1) * split if t < 2 else blocks, attend, 0)
        serve(1)

    tile = 32
    other_half = pl.ds((1 - core) * half, half)
    swap = remote(part.at[other_half], first, core_send, core_recv, (me, partner))
    swap.wait()

    def add_first(i, carry):
        r = pl.ds(pl.multiple_of(i * tile, tile), tile)
        o = pl.ds(pl.multiple_of(core * half + i * tile, tile), tile)
        first[r, :] = (part[o, :].astype(F32) + first[r, :].astype(F32)).astype(BF16)
        return carry

    lax.fori_loop(0, half // tile, add_first, 0)
    copies = []
    for j in range(1, ny):
        to = lax.rem(y + j, ny)
        copies.append(remote(
            first.at[pl.ds(to * piece, piece)], second.at[j - 1], y_send.at[j - 1], y_recv.at[j - 1], (me, to * 2 + core)
        ))
    serve(2)
    for c in copies:
        c.wait()

    def add_second(i, carry):
        r = pl.ds(pl.multiple_of(i * tile, tile), tile)
        s = first[pl.ds(pl.multiple_of(y * piece + i * tile, tile), tile), :].astype(F32)
        for j in range(ny - 1):
            s = s + second[j, r, :].astype(F32)
        o = pl.ds(pl.multiple_of(core * half + y * piece + i * tile, tile), tile)
        mixed[o, :] = (res[r, :].astype(F32) + s).astype(BF16)
        return carry

    lax.fori_loop(0, piece // tile, add_second, 0)
    mine = mixed.at[pl.ds(core * half + y * piece, piece)]
    copies = []
    for j in range(1, ny):
        to = lax.rem(y + j, ny)
        copies.append(remote(mine, mine, back_send.at[j - 1], back_recv.at[j - 1], (me, to * 2 + core)))
    serve(2)
    for j, c in enumerate(copies):
        c.wait_send()
        frm = lax.rem(y + ny - (j + 1), ny)
        theirs = mixed.at[pl.ds(core * half + frm * piece, piece)]
        pltpu.make_async_remote_copy(
            src_ref=theirs, dst_ref=theirs, send_sem=back_send.at[j], recv_sem=back_recv.at[j],
            device_id=(me, partner), device_id_type=MESH,
        ).wait_recv()
    own_half = mixed.at[pl.ds(core * half, half)]
    swap = remote(own_half, own_half, pair_send, pair_recv, (me, partner))
    swap.wait_send()
    their_half = mixed.at[other_half]
    pltpu.make_async_remote_copy(
        src_ref=their_half, dst_ref=their_half, send_sem=pair_send, recv_sem=pair_recv,
        device_id=(me, partner), device_id_type=MESH,
    ).wait_recv()

    def normalise(i, carry):
        r = pl.ds(pl.multiple_of(i * tile, tile), tile)
        m = mixed[r, :].astype(F32)
        mean_sq = jnp.mean(m * m, axis=1, keepdims=True)
        normed[r, :] = (m * lax.rsqrt(mean_sq + EPS) * gain_ref[...]).astype(BF16)
        return carry

    lax.fori_loop(0, rows // tile, normalise, 0)

    serve(2 * (n - 1) - done[0])
    big = rows // 3

    def project(t, which, dst):
        r = slice(t * big, (t + 1) * big)
        dst[r, :] = jnp.dot(normed[r, :], up[which], preferred_element_type=F32).astype(BF16)

    for t in range(3):
        project(t, 0, value)
        serve(1)
    tail = remote(value.at[pl.ds(rows - RIM, RIM)], rim.at[0], rim_send.at[0], rim_recv.at[0], (right, tp))
    head = remote(value.at[pl.ds(0, RIM)], rim.at[1], rim_send.at[1], rim_recv.at[1], (left, tp))
    for t in range(3):
        project(t, 1, gate)
        serve(1)
    tail.wait()
    head.wait()

    taps = taps_ref[...].astype(F32)
    step = 64
    before = rim[0, RIM - 1:RIM, :].astype(F32)

    def label(i, shift):
        return lc[WINDOW + i * step + shift:WINDOW + (i + 1) * step + shift, 0:1]

    for i in range(rows // step):
        r = slice(i * step, (i + 1) * step)
        x = value[r, :].astype(F32)
        after = (value[(i + 1) * step:(i + 1) * step + RIM, :] if (i + 1) * step < rows else rim[1, :, :])[0:1].astype(F32)
        prev = jnp.concatenate([before, x[:-1]], axis=0)
        nxt = jnp.concatenate([x[1:], after], axis=0)
        conv = (
            taps[0:1] * jnp.where(label(i, -1) == label(i, 0), prev, 0.0)
            + taps[1:2] * x
            + taps[2:3] * jnp.where(label(i, 1) == label(i, 0), nxt, 0.0)
        )
        gate[r, :] = (conv * jax.nn.sigmoid(conv) * gate[r, :].astype(F32)).astype(BF16)
        before = x[step - 1:step]
        if i % 4 == 3:
            serve(1)

    per_tp = n // ntp
    mine_rows = pl.ds(core * half, half)
    partner_rows = pl.ds((1 - core) * half, half)
    need = {d: 2 * (n - 1) + (2 * max(d, n - d) if d else 0) for d in range(n)}
    order = sorted(range(n), key=lambda d: need[d])

    def target(owner):
        to = owner // per_tp
        local = lax.rem(owner, per_tp)
        slot = lax.rem(tp - to + ntp, ntp) - 1
        return to, local, slot

    def lower(d):
        owner = place(lax.rem(pos + d, n))
        w = down[pl.ds(pl.multiple_of(owner * block, block), block), :]

        def body(i, carry):
            r = pl.ds(pl.multiple_of(i * big, big), big)
            pd[owner, r, :] = lax.dot_general(
                gate[r, :], w, (((1,), (1,)), ((), ())), preferred_element_type=F32
            ).astype(BF16)
            return carry

        lax.fori_loop(0, 3, body, 0)
        return remote(
            pd.at[owner, partner_rows], box.at[owner], down_send.at[d], down_recv.at[d], (me, partner)
        )

    def reduce(d, c):
        owner = place(lax.rem(pos + d, n))
        c.wait()

        def merge(i, carry):
            r = pl.ds(pl.multiple_of(i * tile, tile), tile)
            o = pl.ds(pl.multiple_of(core * half + i * tile, tile), tile)
            pd[owner, o, :] = (pd[owner, o, :].astype(F32) + box[owner, r, :].astype(F32)).astype(BF16)
            return carry

        lax.fori_loop(0, half // tile, merge, 0, unroll=2)
        to, local, slot = target(owner)

        @pl.when(to != tp)
        def _():
            remote(pd.at[owner, mine_rows], inbox.at[local, slot], out_send.at[d], out_recv.at[local, slot], (me, to))

    waiting = None
    for d in order:
        serve(need[d] - done[0])
        c = lower(d)
        if waiting is not None:
            reduce(*waiting)
        waiting = (d, c)
    reduce(*waiting)
    serve(len(queue))

    span = per_tp * block
    for local in range(per_tp):
        owner = tp * per_tp + local
        for slot in range(ntp - 1):
            ref = inbox.at[local, slot]
            pltpu.make_async_remote_copy(
                src_ref=ref, dst_ref=ref, send_sem=out_send.at[0], recv_sem=out_recv.at[local, slot],
                device_id=(me, partner), device_id_type=MESH,
            ).wait_recv()
        for same in range(2):
            base = (core if same else 1 - core) * half
            slots = range(1, ntp - 1, 2) if same else range(0, ntp - 1, 2)

            def finish(i, carry):
                r = pl.ds(pl.multiple_of(i * tile, tile), tile)
                o = pl.ds(pl.multiple_of(base + i * tile, tile), tile)
                s = sum(inbox[local, slot, r, :].astype(F32) for slot in slots)
                if same:
                    s = s + pd[owner, o, :].astype(F32)
                kept = mixed[o, pl.ds(pl.multiple_of(tp * span, span), span)]
                kept = kept[:, local * block:(local + 1) * block].astype(F32)
                out_ref[o, local * block:(local + 1) * block] = (kept + s).astype(BF16)
                return carry

            lax.fori_loop(0, half // tile, finish, 0)
    for d in range(n):
        owner = place(lax.rem(pos + d, n))
        to, local, slot = target(owner)

        @pl.when(to != tp)
        def _():
            ref = pd.at[owner, mine_rows]
            pltpu.make_async_remote_copy(
                src_ref=ref, dst_ref=ref, send_sem=out_send.at[d], recv_sem=out_recv.at[0, 0],
                device_id=(me, to), device_id_type=MESH,
            ).wait_send()
    for stream in range(4):
        for way in range(2):
            for s in range(n - 1):
                ring(stream, way, s, False).wait_send()


def solution(mesh):
    n, ntp = mesh.shape["sp"], mesh.shape["tp"]

    def per_device(q, k, v, sink, doc, res, wout, gain, wv, wg, taps, wd):
        rows, model = res.shape
        hidden = wv.shape[1]
        block = wv.shape[0]
        ny = ntp // 2
        labels = doc + 1
        lab_row = labels[None, :]
        vm = pl.BlockSpec(memory_space=pltpu.VMEM)
        hbm = pl.BlockSpec(memory_space=pl.ANY)
        smem = pl.BlockSpec(memory_space=pltpu.SMEM)
        dma = pltpu.SemaphoreType.DMA
        kvc = k.shape[1]
        span = model // ntp
        scratch = [
            pltpu.VMEM((2, n * block, hidden), BF16),
            pltpu.VMEM((n * block, hidden), BF16),
            pltpu.VMEM((rows + 2 * WINDOW, kvc), BF16),
            pltpu.VMEM((rows + 2 * WINDOW, kvc), BF16),
            pltpu.VMEM((1, rows + 2 * WINDOW), jnp.int32),
            pltpu.VMEM((rows + 2 * WINDOW, WINDOW), F32),
            pltpu.VMEM((rows, model), BF16),
            pltpu.VMEM((rows // 2, model), BF16),
            pltpu.VMEM((max(ny - 1, 1), rows // 2 // ny, model), BF16),
            pltpu.VMEM((rows, model), BF16),
            pltpu.VMEM((rows, model), BF16),
            pltpu.VMEM((rows, hidden), BF16),
            pltpu.VMEM((rows, hidden), BF16),
            pltpu.VMEM((2, RIM, hidden), BF16),
            pltpu.VMEM((n, rows, block), BF16),
            pltpu.VMEM((n, rows // 2, block), BF16),
            pltpu.VMEM((n // ntp, ntp - 1, rows // 2, block), BF16),
            pltpu.VMEM((rows // 2 // ny, model), BF16),
            dma((4,)),
            dma((4, 2, n - 1)), dma((4, 2, n - 1)),
            dma((3, 2)), dma((3, 2)),
            dma((2,)), dma((2,)),
            dma, dma,
            dma((ny,)), dma((ny,)),
            dma((ny,)), dma((ny,)),
            dma, dma,
            dma((n,)), dma((n,)),
            dma((n,)), dma((n // ntp, ntp - 1)),
        ]
        return pl.pallas_call(
            functools.partial(kernel, n, ntp),
            out_shape=jax.ShapeDtypeStruct((rows, span), BF16),
            in_specs=[vm, vm, vm, smem, vm, hbm, vm, vm, hbm, hbm, vm, hbm],
            out_specs=vm,
            scratch_shapes=scratch,
            compiler_params=pltpu.CompilerParams(
                collective_id=0, has_side_effects=True, vmem_limit_bytes=67043328
            ),
            name="layer",
        )(q, k, v, sink, lab_row, res, wout, gain[None, :], wv, wg, taps, wd)

    placed = (
        P("sp", "tp"), P("sp", "tp"), P("sp", "tp"), P("tp"), P("sp"), P("sp", None),
        P("tp", None), P(), P("sp", "tp"), P("sp", "tp"), P(None, "tp"), P("sp", "tp"),
    )
    return jax.shard_map(
        per_device, mesh=mesh, in_specs=placed, out_specs=P("sp", "tp"), check_vma=False
    )
```

```python
import functools

import jax
import jax.numpy as jnp
from jax import lax
from jax.experimental import pallas as pl
from jax.experimental.pallas import tpu as pltpu
from jax.sharding import PartitionSpec as P

HEAD_DIM = 64
WINDOW = 128
EPS = 1e-06
NEG = -1e30
RIM = 16
MESH = pl.DeviceIdType.MESH
F32 = jnp.float32
BF16 = jnp.bfloat16


def kernel(
    n, ntp,
    q_ref, k_ref, v_ref, sink_ref, lab_row_ref,
    res_hbm, wout_ref, gain_ref, wv_hbm, wg_hbm, taps_ref, wd_hbm,
    out_ref,
    up, down, kx, vx, lx, lc, part, first, second, mixed, normed, value, gate, rim, pd, box, inbox, res,
    loc_sem, ring_send, ring_recv, halo_send, halo_recv, rim_send, rim_recv,
    core_send, core_recv, y_send, y_recv, back_send, back_recv, pair_send, pair_recv,
    down_send, down_recv, out_send, out_recv,
):
    me = lax.axis_index("sp")
    tp = lax.axis_index("tp")
    core = lax.rem(tp, 2)
    y = tp // 2
    ny = ntp // 2
    partner = y * 2 + 1 - core
    rows = q_ref.shape[0]
    half = rows // 2
    piece = half // ny
    block = wv_hbm.shape[0]
    depth = block // 2
    quarter = block // 4

    def place(p):
        h = p // (n // 2)
        return (1 - h) * (2 * p) + h * (2 * n - 1 - 2 * p)

    odd = lax.rem(me, 2)
    pos = (1 - odd) * (me // 2) + odd * ((2 * n - 1 - me) // 2)
    ahead = place(lax.rem(pos + 1, n))
    behind = place(lax.rem(pos + n - 1, n))
    right = lax.rem(me + 1, n)
    left = lax.rem(me + n - 1, n)

    loads = []
    for i, (src, dst) in enumerate((
        (wv_hbm, up.at[0, pl.ds(me * block, block)]),
        (wg_hbm, up.at[1, pl.ds(me * block, block)]),
        (wd_hbm, down.at[pl.ds(me * block, block)]),
        (res_hbm.at[pl.ds(core * half + y * piece, piece)], res),
    )):
        c = pltpu.make_async_copy(src, dst, loc_sem.at[i])
        c.start()
        loads.append(c)

    barrier = pltpu.get_barrier_semaphore()
    peers = [(ahead, tp), (behind, tp), (right, tp), (left, tp)]
    for j in range(1, ntp):
        peers.append((me, lax.rem(tp + j, ntp)))
    for peer in peers:
        pl.semaphore_signal(barrier, inc=1, device_id=peer, device_id_type=MESH)
    for c in loads:
        c.wait()
    pl.semaphore_wait(barrier, len(peers))

    def spot(stream, way, owner):
        if stream < 2:
            return up.at[stream, pl.ds(owner * block + way * depth, depth)]
        return down.at[pl.ds(owner * block + way * depth + (stream - 2) * quarter, quarter)]

    def ring(stream, way, s, arriving):
        shift = s + 1 if arriving else s
        owner = place(lax.rem(pos + n - shift, n)) if way == 0 else place(lax.rem(pos + shift, n))
        ref = spot(stream, way, owner)
        return pltpu.make_async_remote_copy(
            src_ref=ref, dst_ref=ref,
            send_sem=ring_send.at[stream, way, s], recv_sem=ring_recv.at[stream, way, s],
            device_id=(ahead if way == 0 else behind, tp), device_id_type=MESH,
        )

    def begin(stream):
        for way in range(2):
            ring(stream, way, 0, False).start()

    def forward(stream, s, last=False):
        for way in range(2):
            ring(stream, way, s, True).wait_recv()
            if not last:
                ring(stream, way, s + 1, False).start()

    queue = []
    for s in range(n - 1):
        for stream in (0, 1):
            queue.append((stream, s))
    for s in range(n - 1):
        for stream in (2, 3):
            queue.append((stream, s))
    done = [0]

    def serve(count):
        for _ in range(count):
            if done[0] == len(queue):
                return
            stream, s = queue[done[0]]
            done[0] += 1
            forward(stream, s, last=s == n - 2)
            if stream < 2 and s == n - 2:
                begin(stream + 2)

    halo = []

    def remote(src, dst, send, recv, where):
        c = pltpu.make_async_remote_copy(
            src_ref=src, dst_ref=dst, send_sem=send, recv_sem=recv, device_id=where, device_id_type=MESH
        )
        c.start()
        return c

    ends = pl.ds(rows - WINDOW, WINDOW)
    starts = pl.ds(0, WINDOW)
    low, high = pl.ds(0, WINDOW), pl.ds(rows + WINDOW, WINDOW)
    for i, (src, dst) in enumerate(((k_ref, kx), (v_ref, vx))):
        halo.append(remote(src.at[ends], dst.at[low], halo_send.at[i, 0], halo_recv.at[i, 0], (right, tp)))
        halo.append(remote(src.at[starts], dst.at[high], halo_send.at[i, 1], halo_recv.at[i, 1], (left, tp)))
    halo.append(remote(lab_row_ref.at[:, ends], lx.at[:, low], halo_send.at[2, 0], halo_recv.at[2, 0], (right, tp)))
    halo.append(remote(lab_row_ref.at[:, starts], lx.at[:, high], halo_send.at[2, 1], halo_recv.at[2, 1], (left, tp)))
    begin(0)
    begin(1)
    inner = pl.ds(WINDOW, rows)
    kx[inner, :] = k_ref[...]
    vx[inner, :] = v_ref[...]
    lx[:, inner] = lab_row_ref[...]
    for c in halo:
        c.wait()
    lx[:, low] = jnp.where(me == 0, -1, lx[:, low])
    lx[:, high] = jnp.where(me == n - 1, -1, lx[:, high])
    for i in range(rows // WINDOW + 2):
        chunk = slice(i * WINDOW, (i + 1) * WINDOW)
        square = jnp.broadcast_to(lx[0:1, chunk].astype(F32), (WINDOW, WINDOW))
        lc[chunk, :] = jnp.transpose(square)

    kv_local = k_ref.shape[1] // HEAD_DIM
    per_kv = q_ref.shape[1] // k_ref.shape[1]
    blocks = rows // WINDOW
    model = wout_ref.shape[1]

    def attend(b, carry):
        here = pl.ds(pl.multiple_of(b * WINDOW, WINDOW), WINDOW)
        wide = pl.ds(pl.multiple_of(b * WINDOW, WINDOW), 3 * WINDOW)
        q = q_ref[here, :]
        kw = kx[wide, :]
        vw = vx[wide, :]
        lab_k = lx[0:1, wide].astype(F32)
        lab_q = lc[pl.ds(pl.multiple_of(b * WINDOW + WINDOW, WINDOW), WINDOW), 0:1]
        key = lax.broadcasted_iota(jnp.int32, (WINDOW, 3 * WINDOW), 1) - WINDOW
        query = lax.broadcasted_iota(jnp.int32, (WINDOW, 3 * WINDOW), 0)
        allowed = (jnp.abs(key - query) <= WINDOW) & (lab_q == lab_k)
        results = []
        for g in range(kv_local):
            k = kw[:, g * HEAD_DIM:(g + 1) * HEAD_DIM]
            v = vw[:, g * HEAD_DIM:(g + 1) * HEAD_DIM]
            for j in range(per_kv):
                h = g * per_kv + j
                qh = q[:, h * HEAD_DIM:(h + 1) * HEAD_DIM]
                score = lax.dot_general(
                    qh, k, (((1,), (1,)), ((), ())), preferred_element_type=F32
                ) * HEAD_DIM ** (-0.5)
                score = jnp.where(allowed, score, NEG)
                sink = sink_ref[h]
                highest = jnp.maximum(jnp.max(score, axis=1, keepdims=True), sink)
                raw = jnp.where(allowed, jnp.exp(score - highest), 0.0)
                total = jnp.sum(raw, axis=1, keepdims=True) + jnp.exp(sink - highest)
                probs = (raw / total).astype(BF16)
                results.append(jnp.dot(probs, v, preferred_element_type=F32).astype(BF16))
        attended = jnp.concatenate(results, axis=1)
        part[here, :] = jnp.dot(attended, wout_ref[...], preferred_element_type=F32).astype(BF16)
        return carry

    split = blocks // 3
    for t in range(3):
        lax.fori_loop(t * split, (t + 1) * split if t < 2 else blocks, attend, 0)
        serve(2 if t == 1 else 1)

    tile = 32
    other_half = pl.ds((1 - core) * half, half)
    swap = remote(part.at[other_half], first, core_send, core_recv, (me, partner))
    swap.wait()

    def add_first(i, carry):
        r = pl.ds(pl.multiple_of(i * tile, tile), tile)
        o = pl.ds(pl.multiple_of(core * half + i * tile, tile), tile)
        first[r, :] = (part[o, :].astype(F32) + first[r, :].astype(F32)).astype(BF16)
        return carry

    lax.fori_loop(0, half // tile, add_first, 0)
    copies = []
    for j in range(1, ny):
        to = lax.rem(y + j, ny)
        copies.append(remote(
            first.at[pl.ds(to * piece, piece)], second.at[j - 1], y_send.at[j - 1], y_recv.at[j - 1], (me, to * 2 + core)
        ))
    serve(2)
    for c in copies:
        c.wait()

    def add_second(i, carry):
        r = pl.ds(pl.multiple_of(i * tile, tile), tile)
        s = first[pl.ds(pl.multiple_of(y * piece + i * tile, tile), tile), :].astype(F32)
        for j in range(ny - 1):
            s = s + second[j, r, :].astype(F32)
        o = pl.ds(pl.multiple_of(core * half + y * piece + i * tile, tile), tile)
        mixed[o, :] = (res[r, :].astype(F32) + s).astype(BF16)
        return carry

    lax.fori_loop(0, piece // tile, add_second, 0)
    mine = mixed.at[pl.ds(core * half + y * piece, piece)]
    copies = []
    for j in range(1, ny):
        to = lax.rem(y + j, ny)
        copies.append(remote(mine, mine, back_send.at[j - 1], back_recv.at[j - 1], (me, to * 2 + core)))
    serve(2)
    for j, c in enumerate(copies):
        c.wait_send()
        frm = lax.rem(y + ny - (j + 1), ny)
        theirs = mixed.at[pl.ds(core * half + frm * piece, piece)]
        pltpu.make_async_remote_copy(
            src_ref=theirs, dst_ref=theirs, send_sem=back_send.at[j], recv_sem=back_recv.at[j],
            device_id=(me, partner), device_id_type=MESH,
        ).wait_recv()
    own_half = mixed.at[pl.ds(core * half, half)]
    swap = remote(own_half, own_half, pair_send, pair_recv, (me, partner))
    swap.wait_send()
    their_half = mixed.at[other_half]
    pltpu.make_async_remote_copy(
        src_ref=their_half, dst_ref=their_half, send_sem=pair_send, recv_sem=pair_recv,
        device_id=(me, partner), device_id_type=MESH,
    ).wait_recv()

    def normalise(i, carry):
        r = pl.ds(pl.multiple_of(i * tile, tile), tile)
        m = mixed[r, :].astype(F32)
        mean_sq = jnp.mean(m * m, axis=1, keepdims=True)
        normed[r, :] = (m * lax.rsqrt(mean_sq + EPS) * gain_ref[...]).astype(BF16)
        return carry

    lax.fori_loop(0, rows // tile, normalise, 0)

    serve(2 * (n - 1) - done[0])
    big = rows // 3

    def project(t, which, dst):
        r = slice(t * big, (t + 1) * big)
        dst[r, :] = jnp.dot(normed[r, :], up[which], preferred_element_type=F32).astype(BF16)

    for t in range(3):
        project(t, 0, value)
        serve(1)
    tail = remote(value.at[pl.ds(rows - RIM, RIM)], rim.at[0], rim_send.at[0], rim_recv.at[0], (right, tp))
    head = remote(value.at[pl.ds(0, RIM)], rim.at[1], rim_send.at[1], rim_recv.at[1], (left, tp))
    for t in range(3):
        project(t, 1, gate)
        serve(1)
    tail.wait()
    head.wait()

    taps = taps_ref[...].astype(F32)
    step = 64
    before = rim[0, RIM - 1:RIM, :].astype(F32)

    def label(i, shift):
        return lc[WINDOW + i * step + shift:WINDOW + (i + 1) * step + shift, 0:1]

    for i in range(rows // step):
        r = slice(i * step, (i + 1) * step)
        x = value[r, :].astype(F32)
        after = (value[(i + 1) * step:(i + 1) * step + RIM, :] if (i + 1) * step < rows else rim[1, :, :])[0:1].astype(F32)
        prev = jnp.concatenate([before, x[:-1]], axis=0)
        nxt = jnp.concatenate([x[1:], after], axis=0)
        conv = (
            taps[0:1] * jnp.where(label(i, -1) == label(i, 0), prev, 0.0)
            + taps[1:2] * x
            + taps[2:3] * jnp.where(label(i, 1) == label(i, 0), nxt, 0.0)
        )
        gate[r, :] = (conv * jax.nn.sigmoid(conv) * gate[r, :].astype(F32)).astype(BF16)
        before = x[step - 1:step]
        if i % 3 == 2:
            serve(1)

    per_tp = n // ntp
    mine_rows = pl.ds(core * half, half)
    partner_rows = pl.ds((1 - core) * half, half)
    units = []
    for d in range(n):
        if d in (1, n - 1) and n > 2:
            units.append((2 * (n - 1) + 2 * (n - d), d, 0, 1))
            units.append((2 * (n - 1) + 2 * d, d, 1, 1))
        else:
            units.append((2 * (n - 1) + (2 * max(d, n - d) if d else 0), d, 0, 2))
    units.sort()

    def target(owner):
        to = owner // per_tp
        local = lax.rem(owner, per_tp)
        slot = lax.rem(tp - to + ntp, ntp) - 1
        return to, local, slot

    def lower(u):
        _, d, way, count = units[u]
        owner = place(lax.rem(pos + d, n))
        w = down[pl.ds(pl.multiple_of(owner * block + way * depth, depth), count * depth), :]

        def body(i, carry):
            r = pl.ds(pl.multiple_of(i * big, big), big)
            product = lax.dot_general(
                gate[r, :], w, (((1,), (1,)), ((), ())), preferred_element_type=F32
            ).astype(BF16)
            for j in range(count):
                pd[owner, way + j, r, :] = product[:, j * depth:(j + 1) * depth]
            return carry

        lax.fori_loop(0, 3, body, 0)
        return remote(
            pd.at[owner, pl.ds(way, count), partner_rows], box.at[owner, pl.ds(way, count)],
            down_send.at[u], down_recv.at[u], (me, partner),
        )

    def reduce(u, c):
        _, d, way, count = units[u]
        owner = place(lax.rem(pos + d, n))
        c.wait()

        def merge(i, carry):
            r = pl.ds(pl.multiple_of(i * tile, tile), tile)
            o = pl.ds(pl.multiple_of(core * half + i * tile, tile), tile)
            for j in range(way, way + count):
                pd[owner, j, o, :] = (pd[owner, j, o, :].astype(F32) + box[owner, j, r, :].astype(F32)).astype(BF16)
            return carry

        lax.fori_loop(0, half // tile, merge, 0, unroll=2)
        to, local, slot = target(owner)

        @pl.when(to != tp)
        def _():
            remote(
                pd.at[owner, pl.ds(way, count), mine_rows], inbox.at[local, slot, pl.ds(way, count)],
                out_send.at[u], out_recv.at[local, slot], (me, to),
            )

    waiting = None
    for u in range(len(units)):
        serve(units[u][0] - done[0])
        c = lower(u)
        if waiting is not None:
            reduce(*waiting)
        waiting = (u, c)
    reduce(*waiting)
    serve(len(queue))

    span = per_tp * block
    for local in range(per_tp):
        owner = tp * per_tp + local
        for slot in range(ntp - 1):
            ref = inbox.at[local, slot]
            pltpu.make_async_remote_copy(
                src_ref=ref, dst_ref=ref, send_sem=out_send.at[0], recv_sem=out_recv.at[local, slot],
                device_id=(me, partner), device_id_type=MESH,
            ).wait_recv()
        for same in range(2):
            base = (core if same else 1 - core) * half
            slots = range(1, ntp - 1, 2) if same else range(0, ntp - 1, 2)

            def finish(i, carry):
                r = pl.ds(pl.multiple_of(i * tile, tile), tile)
                o = pl.ds(pl.multiple_of(base + i * tile, tile), tile)
                kept = mixed[o, pl.ds(pl.multiple_of(tp * span, span), span)]
                for j in range(2):
                    s = sum(inbox[local, slot, j, r, :].astype(F32) for slot in slots)
                    if same:
                        s = s + pd[owner, j, o, :].astype(F32)
                    cols = slice(local * block + j * depth, local * block + (j + 1) * depth)
                    out_ref[o, cols] = (kept[:, cols].astype(F32) + s).astype(BF16)
                return carry

            lax.fori_loop(0, half // tile, finish, 0)
    for u, (_, d, way, count) in enumerate(units):
        owner = place(lax.rem(pos + d, n))
        to, local, slot = target(owner)

        @pl.when(to != tp)
        def _():
            ref = pd.at[owner, pl.ds(way, count), mine_rows]
            pltpu.make_async_remote_copy(
                src_ref=ref, dst_ref=ref, send_sem=out_send.at[u], recv_sem=out_recv.at[0, 0],
                device_id=(me, to), device_id_type=MESH,
            ).wait_send()
    for stream in range(4):
        for way in range(2):
            for s in range(n - 1):
                ring(stream, way, s, False).wait_send()


def solution(mesh):
    n, ntp = mesh.shape["sp"], mesh.shape["tp"]

    def per_device(q, k, v, sink, doc, res, wout, gain, wv, wg, taps, wd):
        rows, model = res.shape
        hidden = wv.shape[1]
        block = wv.shape[0]
        ny = ntp // 2
        labels = doc + 1
        lab_row = labels[None, :]
        vm = pl.BlockSpec(memory_space=pltpu.VMEM)
        hbm = pl.BlockSpec(memory_space=pl.ANY)
        smem = pl.BlockSpec(memory_space=pltpu.SMEM)
        dma = pltpu.SemaphoreType.DMA
        kvc = k.shape[1]
        span = model // ntp
        scratch = [
            pltpu.VMEM((2, n * block, hidden), BF16),
            pltpu.VMEM((n * block, hidden), BF16),
            pltpu.VMEM((rows + 2 * WINDOW, kvc), BF16),
            pltpu.VMEM((rows + 2 * WINDOW, kvc), BF16),
            pltpu.VMEM((1, rows + 2 * WINDOW), jnp.int32),
            pltpu.VMEM((rows + 2 * WINDOW, WINDOW), F32),
            pltpu.VMEM((rows, model), BF16),
            pltpu.VMEM((rows // 2, model), BF16),
            pltpu.VMEM((max(ny - 1, 1), rows // 2 // ny, model), BF16),
            pltpu.VMEM((rows, model), BF16),
            pltpu.VMEM((rows, model), BF16),
            pltpu.VMEM((rows, hidden), BF16),
            pltpu.VMEM((rows, hidden), BF16),
            pltpu.VMEM((2, RIM, hidden), BF16),
            pltpu.VMEM((n, 2, rows, block // 2), BF16),
            pltpu.VMEM((n, 2, rows // 2, block // 2), BF16),
            pltpu.VMEM((n // ntp, ntp - 1, 2, rows // 2, block // 2), BF16),
            pltpu.VMEM((rows // 2 // ny, model), BF16),
            dma((4,)),
            dma((4, 2, n - 1)), dma((4, 2, n - 1)),
            dma((3, 2)), dma((3, 2)),
            dma((2,)), dma((2,)),
            dma, dma,
            dma((ny,)), dma((ny,)),
            dma((ny,)), dma((ny,)),
            dma, dma,
            dma((n + 2,)), dma((n + 2,)),
            dma((n + 2,)), dma((n // ntp, ntp - 1)),
        ]
        return pl.pallas_call(
            functools.partial(kernel, n, ntp),
            out_shape=jax.ShapeDtypeStruct((rows, span), BF16),
            in_specs=[vm, vm, vm, smem, vm, hbm, vm, vm, hbm, hbm, vm, hbm],
            out_specs=vm,
            scratch_shapes=scratch,
            compiler_params=pltpu.CompilerParams(
                collective_id=0, has_side_effects=True, vmem_limit_bytes=67043328
            ),
            name="layer",
        )(q, k, v, sink, lab_row, res, wout, gain[None, :], wv, wg, taps, wd)

    placed = (
        P("sp", "tp"), P("sp", "tp"), P("sp", "tp"), P("tp"), P("sp"), P("sp", None),
        P("tp", None), P(), P("sp", "tp"), P("sp", "tp"), P(None, "tp"), P("sp", "tp"),
    )
    return jax.shard_map(
        per_device, mesh=mesh, in_specs=placed, out_specs=P("sp", "tp"), check_vma=False
    )
```
